32 devices in a mesh: ep: 4 (over z), tp: 8 (over y, x, core).
Axes of the slice: x: 2, y: 2, z: 4, core: 2. Of those that a mesh axis runs over, the one named last changes fastest.
Arguments:
- tokens: bfloat16 [256, 4096], P('ep', 'tp'), may hold values from -24 to 24, as said below
- state_real: float32 [256, 128, 64], P('ep', 'tp'), may hold values from -3 to 3
- state_imag: float32 [256, 128, 64], P('ep', 'tp'), may hold values from -3 to 3
- mix_gain: bfloat16 [4096], replicated, may hold values from 0.099609375 to 1.8984375
- in_weight: bfloat16 [2048, 4096], P('tp'), may hold values from -0.09375 to 0.09375
- eig_real: float32 [128, 64], P('tp'), may hold values from -1 to -0.1
- eig_imag: float32 [128, 64], P('tp'), may hold values from 0 to 200
- log_step: float32 [128], P('tp'), may hold values from -4 to 0
- input_real: float32 [128, 64, 16], P('tp'), may hold values from -1 to 1
- input_imag: float32 [128, 64, 16], P('tp'), may hold values from -1 to 1
- output_matrix_real: float32 [128, 16, 64], P('tp'), may hold values from -0.5 to 0.5
- output_matrix_imag: float32 [128, 16, 64], P('tp'), may hold values from -0.5 to 0.5
- skip_weight: float32 [2048], P('tp'), may hold values from -3 to 3
- glu_weight: bfloat16 [2048, 2048], P('tp'), may hold values from -0.375 to 0.375
- glu_bias: float32 [2048], P('tp'), may hold values from -3 to 3
- out_weight: bfloat16 [2048, 4096], P('tp'), may hold values from -0.25 to 0.25
- moe_gain: bfloat16 [4096], replicated, may hold values from 0.099609375 to 1.8984375
- routes: int32 [256, 2], P('ep'), may hold values from 0 to 7, all different within a row; in each aligned block of 64 rows (0 to 63, 64 to 127, ...) at most 24 rows name the same one
- route_weight: float32 [256, 2], P('ep'), may hold values from 0.2 to 1
- gate_weight: bfloat16 [8, 2048, 4096], P('ep', 'tp'), may hold values from -0.09375 to 0.09375
- up_weight: bfloat16 [8, 2048, 4096], P('ep', 'tp'), may hold values from -0.09375 to 0.09375
- down_weight: bfloat16 [8, 2048, 4096], P('ep', 'tp'), may hold values from -0.125 to 0.125
Outputs:
- result: bfloat16 [256, 4096], P('ep', 'tp')
- updated_state_real: float32 [256, 128, 64], P('ep', 'tp')
- updated_state_imag: float32 [256, 128, 64], P('ep', 'tp')
The draws below stay inside these ranges and needn't reach their ends.
Inputs may be any that keep to these rules, and one draw needn't show every extreme that they name: `routes`: each row names 2 different experts. Among the rows of one index of ep, no expert is named by more than 24 rows, a bound that some expert reaches in some such blocks. `tokens`: feature blocks of the stream have scales that differ by up to a factor of ten.
All inputs are finite; a program needn't handle non-finite values.
Results may differ from the reference program's by a relative error of at most 0.013.
Values may be sent and summed in bfloat16 or wider, within the bound.
A program may use at most 64 MiB of HBM per device.

```python
import math
import jax
import jax.numpy as jnp
import numpy as np
from jax import lax

D = 4096
S5_GROUP = 16
S5_GROUPS = 128
S5_STATE = 64
S5_WIDTH = 2048
D_EXPERT = 2048
EXPERTS = 8
TOP = 2
B_DEV = 64
TOKENS = 256
CAP = 24
N_EP = 4
N_TP = 8


def draw_tokens(key, part):
    key_base = jax.random.fold_in(key, 11)
    key_scale = jax.random.fold_in(key, 12)
    block_scale = jnp.exp(jax.random.uniform(key_scale, (32,), jnp.float32, math.log(0.3), math.log(3.0)))
    col_scale = jnp.repeat(block_scale, D // 32)
    base = jnp.clip(jax.random.normal(key_base, (TOKENS, D), jnp.float32), -4.0, 4.0)
    return (base * col_scale[None, :]).astype(jnp.bfloat16)


def steps_of(stream_key, dims, shards, low, top_value):
    loudness = 1.0
    for axis_at, parts in shards:
        heights = jax.random.uniform(jax.random.fold_in(jax.random.fold_in(stream_key, 6), axis_at), (parts,), jnp.float32, low / len(shards), top_value / len(shards))
        loudness = loudness * jnp.repeat(jnp.exp(heights), dims[axis_at] // parts).reshape((-1,) + (1,) * (len(dims) - 1 - axis_at))
    return loudness


def shared_out(key, own, number, rows, amount, top, reach, skew):
    ranking = jax.random.permutation(key, amount)
    crowded, usual = portions_of(amount, rows * top, reach, skew, True), portions_of(amount, rows * top, reach, skew, False)
    places = jnp.arange(amount)

    def named(sizes, rotation):
        used = int((sizes > 0).sum())
        fixed = max(1, used // 4)
        passed = fixed + (places - fixed + rotation * (used - fixed)) % max(1, amount - fixed)
        return jnp.zeros((amount,), jnp.int32).at[ranking[jnp.where(places < fixed, places, passed)]].set(jnp.asarray(sizes, jnp.int32))

    sizes = jnp.where(number % 4 == 0, named(crowded, number // 4), named(usual, number - number // 4 - 1))
    mixed = jax.random.permutation(jax.random.fold_in(own, 3), amount)
    source_of, sink = mixed[0:amount // 2 * 2:2], mixed[1:amount // 2 * 2:2]
    margin = jnp.minimum(sizes[source_of] - 1, reach - sizes[sink]) // 2
    margin = jnp.where((source_of == ranking[0]) | (sink == ranking[0]) | (sizes[sink] == 0), 0, jnp.maximum(margin, 0))
    passed = jax.random.randint(jax.random.fold_in(own, 4), (amount // 2,), 0, 1 << 20) % (margin + 1)
    sizes = sizes.at[source_of].add(-passed).at[sink].add(passed)
    members = jnp.searchsorted(jnp.cumsum(sizes), jnp.arange(rows * top), side="right").astype(jnp.int32)
    listing = members.reshape(top, rows).T
    listing = listing[jax.random.permutation(jax.random.fold_in(own, 1), rows)]
    rotation = jax.random.randint(jax.random.fold_in(own, 2), (rows, 1), 0, top)
    return jnp.take_along_axis(listing, (jnp.arange(top)[None, :] + rotation) % top, axis=1)


def portions_of(count, total, most, slope, full):
    portions = [(1 << 20) // math.isqrt(rank ** slope) + 1 for rank in range(1, count + 1)]
    largest = most if full else min(most, max(-(-total // count), total * portions[0] // sum(portions)))
    least = 1 if total - largest >= count - 1 else 0
    holding, spare = [largest] + [least] * (count - 1), total - largest - least * (count - 1)
    while spare > 0:
        free = [i for i in range(1, count) if holding[i] < largest] or [i for i in range(1, count) if holding[i] < most]
        whole, budget = sum([portions[i] for i in free]), spare
        for i in free:
            addition = min(most - holding[i], max(1, budget * portions[i] // whole), spare)
            holding[i] = holding[i] + addition
            spare = spare - addition
    return np.array(holding)


def bell_draw(rng, extent, width, limit, shards=(), held_as=jnp.bfloat16):
    array = width * jax.random.normal(rng, extent, jnp.float32)
    if shards:
        array = array * steps_of(rng, extent, shards, -0.22, 0.18)
    return jnp.clip(array, -limit, limit).astype(held_as)


def setup_inputs(seed: int = 0) -> dict:
    streams_of = jax.random.split(jax.random.key(seed), 23)
    tokens = draw_tokens(jax.random.fold_in(streams_of[22], 71), 0)
    state_real = bell_draw(streams_of[1], (TOKENS, S5_GROUPS, S5_STATE), 0.5, 3.0, ((0, 4), (1, 8)), jnp.float32)
    state_imag = bell_draw(streams_of[2], (TOKENS, S5_GROUPS, S5_STATE), 0.5, 3.0, ((0, 4), (1, 8)), jnp.float32)
    mix_gain = jnp.clip(1.0 + 0.18 * jax.random.normal(streams_of[3], (D,), jnp.float32), 0.099609375, 1.8984375).astype(jnp.bfloat16)
    in_weight = bell_draw(streams_of[4], (S5_WIDTH, D), D ** -0.5, 0.09375, ((0, 8),))
    eig_real = jnp.clip(-1.0 + 0.9 * jax.random.uniform(streams_of[5], (S5_GROUPS, S5_STATE), jnp.float32) ** steps_of(streams_of[5], (S5_GROUPS, S5_STATE), ((0, 8),), -0.2, 0.2), -1.0, -0.1)
    eig_imag = jnp.clip(200.0 * jax.random.uniform(streams_of[6], (S5_GROUPS, S5_STATE), jnp.float32) ** steps_of(streams_of[6], (S5_GROUPS, S5_STATE), ((0, 8),), -0.2, 0.2), 0.0, 200.0)
    log_step = jnp.clip(-4.0 + 4.0 * jax.random.uniform(streams_of[7], (S5_GROUPS,), jnp.float32) ** steps_of(streams_of[7], (S5_GROUPS,), ((0, 8),), -0.2, 0.2), -4.0, 0.0)
    input_real = bell_draw(streams_of[8], (S5_GROUPS, S5_STATE, S5_GROUP), (2 * S5_GROUP) ** -0.5, 1.0, ((0, 8),), jnp.float32)
    input_imag = bell_draw(streams_of[9], (S5_GROUPS, S5_STATE, S5_GROUP), (2 * S5_GROUP) ** -0.5, 1.0, ((0, 8),), jnp.float32)
    output_matrix_real = bell_draw(streams_of[10], (S5_GROUPS, S5_GROUP, S5_STATE), (2 * S5_STATE) ** -0.5, 0.5, ((0, 8),), jnp.float32)
    output_matrix_imag = bell_draw(streams_of[11], (S5_GROUPS, S5_GROUP, S5_STATE), (2 * S5_STATE) ** -0.5, 0.5, ((0, 8),), jnp.float32)
    skip_weight = bell_draw(streams_of[12], (S5_WIDTH,), 0.5, 3.0, ((0, 8),), jnp.float32)
    glu_weight = bell_draw(streams_of[13], (S5_WIDTH, S5_WIDTH), (S5_WIDTH // 8) ** -0.5, 0.375, ((0, 8),))
    glu_bias = bell_draw(streams_of[14], (S5_WIDTH,), 1.0, 3.0, ((0, 8),), jnp.float32)
    out_weight = bell_draw(streams_of[15], (S5_WIDTH, D), (S5_WIDTH // 4) ** -0.5, 0.25, ((0, 8),))
    moe_gain = jnp.clip(1.0 + 0.18 * jax.random.normal(streams_of[16], (D,), jnp.float32), 0.099609375, 1.8984375).astype(jnp.bfloat16)
    routes_keys = jax.random.split(jax.random.fold_in(streams_of[17], 1), TOKENS // B_DEV)
    routes_turns = jax.random.permutation(jax.random.fold_in(streams_of[17], 3), TOKENS // B_DEV)
    routes = jax.vmap(lambda own, number: shared_out(jax.random.fold_in(streams_of[17], 2), own, number, B_DEV, EXPERTS, TOP, CAP, 2))(routes_keys, routes_turns).reshape((TOKENS, TOP))
    route_weight = jnp.clip(0.2 + 0.8 * jax.random.uniform(streams_of[18], (TOKENS, TOP), jnp.float32) ** steps_of(streams_of[18], (TOKENS, TOP), ((0, 4),), -0.2, 0.2), 0.2, 1.0)
    gate_weight = bell_draw(streams_of[19], (EXPERTS, D_EXPERT, D), D ** -0.5, 0.09375, ((0, 4), (1, 8)))
    up_weight = bell_draw(streams_of[20], (EXPERTS, D_EXPERT, D), D ** -0.5, 0.09375, ((0, 4), (1, 8)))
    down_weight = bell_draw(streams_of[21], (EXPERTS, D_EXPERT, D), D_EXPERT ** -0.5, 0.125, ((0, 4), (1, 8)))
    return {"tokens": tokens, "state_real": state_real, "state_imag": state_imag, "mix_gain": mix_gain, "in_weight": in_weight, "eig_real": eig_real, "eig_imag": eig_imag, "log_step": log_step, "input_real": input_real, "input_imag": input_imag, "output_matrix_real": output_matrix_real, "output_matrix_imag": output_matrix_imag, "skip_weight": skip_weight, "glu_weight": glu_weight, "glu_bias": glu_bias, "out_weight": out_weight, "moe_gain": moe_gain, "routes": routes, "route_weight": route_weight, "gate_weight": gate_weight, "up_weight": up_weight, "down_weight": down_weight}


norm_eps = 1e-06

def ssm_step(driven, state_real, state_imag, eig_real, eig_imag, log_step, input_real, input_imag, output_matrix_real, output_matrix_imag, skip_weight):
    highest_precision = lax.Precision.HIGHEST
    count_of_rows = driven.shape[0]
    groups = eig_real.shape[0]
    group_width = input_real.shape[2]
    time_step = jnp.exp(log_step)[:, None]
    magnitude = jnp.exp(eig_real * time_step)
    angle_now = eig_imag * time_step
    bar_real = magnitude * jnp.cos(angle_now)
    bar_imag = magnitude * jnp.sin(angle_now)
    modulus = eig_real * eig_real + eig_imag * eig_imag
    fac_real = ((bar_real - 1.0) * eig_real + bar_imag * eig_imag) / modulus
    fac_imag = (bar_imag * eig_real - (bar_real - 1.0) * eig_imag) / modulus
    ib_real = fac_real[..., None] * input_real - fac_imag[..., None] * input_imag
    ib_imag = fac_real[..., None] * input_imag + fac_imag[..., None] * input_real
    grouped = driven.astype(jnp.float32).reshape(count_of_rows, groups, group_width)
    push_real = jnp.einsum('gpc,ngc->ngp', ib_real, grouped, precision=highest_precision)
    push_imag = jnp.einsum('gpc,ngc->ngp', ib_imag, grouped, precision=highest_precision)
    updated_state_real = bar_real[None] * state_real - bar_imag[None] * state_imag + push_real
    updated_state_imag = bar_real[None] * state_imag + bar_imag[None] * state_real + push_imag
    state_readout = jnp.einsum('jiy,sjy->sji', output_matrix_real, updated_state_real, precision=highest_precision) - jnp.einsum('jiy,sjy->sji', output_matrix_imag, updated_state_imag, precision=highest_precision)
    state_readout = state_readout.reshape(count_of_rows, groups * group_width) + skip_weight[None, :] * driven.astype(jnp.float32)
    activated = jax.nn.gelu(state_readout).astype(jnp.bfloat16)
    return (updated_state_real, updated_state_imag, activated)

def block_sum(left_side, right_side, block_count):
    block_width = left_side.shape[1] // block_count
    left_blocks = left_side.reshape(left_side.shape[0], block_count, block_width).transpose(1, 0, 2)
    right_blocks = right_side.reshape(block_count, block_width, right_side.shape[1])

    def add_block(running, operands):
        partial_value = jnp.dot(operands[0], operands[1], preferred_element_type=jnp.float32).astype(jnp.bfloat16)
        return (running + partial_value.astype(jnp.float32), None)
    start_sum = jnp.zeros((left_side.shape[0], right_side.shape[1]), jnp.float32)
    running, _ = lax.scan(add_block, start_sum, (left_blocks, right_blocks))
    return running

def reference(tokens, state_real, state_imag, mix_gain, in_weight, eig_real, eig_imag, log_step, input_real, input_imag, output_matrix_real, output_matrix_imag, skip_weight, glu_weight, glu_bias, out_weight, moe_gain, routes, route_weight, gate_weight, up_weight, down_weight):
    token_float = tokens.astype(jnp.float32)
    first_scale = lax.rsqrt(lax.optimization_barrier(jnp.mean(token_float * token_float, axis=1, keepdims=True)) + norm_eps)
    normed = (token_float * first_scale * mix_gain.astype(jnp.float32)).astype(jnp.bfloat16)
    driven = jnp.dot(normed, in_weight.T, preferred_element_type=jnp.float32).astype(jnp.bfloat16)
    updated_state_real, updated_state_imag, activated = ssm_step(driven, state_real, state_imag, eig_real, eig_imag, log_step, input_real, input_imag, output_matrix_real, output_matrix_imag, skip_weight)
    gate_pre = jnp.dot(activated, glu_weight.T, preferred_element_type=jnp.float32) + glu_bias
    glued = (activated.astype(jnp.float32) * jax.nn.sigmoid(gate_pre)).astype(jnp.bfloat16)
    mixed = block_sum(glued, out_weight, N_TP)
    residual = (token_float + mixed).astype(jnp.bfloat16)
    resid_float = residual.astype(jnp.float32)
    second_scale = lax.rsqrt(lax.optimization_barrier(jnp.mean(resid_float * resid_float, axis=1, keepdims=True)) + norm_eps)
    expert_in = (resid_float * second_scale * moe_gain.astype(jnp.float32)).astype(jnp.bfloat16)
    experts = gate_weight.shape[0]
    token_count = routes.shape[0]
    per_block = token_count // N_EP
    chosen = routes.reshape(N_EP, per_block * TOP)
    onehot = (chosen[..., None] == jnp.arange(experts, dtype=jnp.int32)[None, None, :]).astype(jnp.int32)
    rank_index = lax.optimization_barrier(jnp.sum((jnp.cumsum(onehot, axis=1) - onehot) * onehot, axis=2))
    source = jnp.arange(N_EP, dtype=jnp.int32)[:, None]
    slot_index = (chosen * (N_EP * CAP) + source * CAP + rank_index).reshape(token_count, TOP).astype(jnp.int32)
    buffer = jnp.zeros((experts * N_EP * CAP, expert_in.shape[1]), jnp.bfloat16)
    buffer = buffer.at[slot_index.reshape(-1)].set(jnp.repeat(expert_in, TOP, axis=0))
    buffer = buffer.reshape(experts, N_EP * CAP, expert_in.shape[1])

    def run_expert(expert_item):
        expert_rows, gate_rows, up_rows, down_rows = expert_item
        gate_sum = jnp.dot(expert_rows, gate_rows.T, preferred_element_type=jnp.float32)
        up_sum = jnp.dot(expert_rows, up_rows.T, preferred_element_type=jnp.float32)
        hidden_width = (jax.nn.silu(gate_sum) * up_sum).astype(jnp.bfloat16)
        return block_sum(hidden_width, down_rows, N_TP).astype(jnp.bfloat16)
    results = lax.map(run_expert, (buffer, gate_weight, up_weight, down_weight))
    flattened = results.reshape(experts * N_EP * CAP, expert_in.shape[1])
    picked = flattened[slot_index]
    result = (resid_float + lax.optimization_barrier(jnp.sum(route_weight[..., None] * picked.astype(jnp.float32), axis=1))).astype(jnp.bfloat16)
    return (result, updated_state_real, updated_state_imag)
```

```python
import functools

import jax
import jax.numpy as jnp
from jax import lax
from jax.experimental import pallas as pl
from jax.experimental.pallas import tpu as pltpu
from jax.sharding import PartitionSpec as P

norm_eps = 1e-06
MESH = pl.DeviceIdType.MESH
F32 = jnp.float32
BF16 = jnp.bfloat16


def dot_nt(a, b):
    return lax.dot_general(a, b, (((1,), (1,)), ((), ())), preferred_element_type=F32)


def dot_nn(a, b):
    return lax.dot_general(a, b, (((1,), (0,)), ((), ())), preferred_element_type=F32)


def layer_kernel(
    n_ep, n_tp, capacity,
    tok, mix_gain, moe_gain, routes, route_weight, eig_real, eig_imag, log_step,
    in_real, in_imag, out_real, out_imag, skip_weight, glu_bias,
    state_real, state_imag, in_weight, glu_weight, out_weight, gate_weight, up_weight, down_weight,
    result, new_real, new_imag,
    tok_all, act_all, sib_send_a, sib_recv_a, rem_send_a, rem_recv_a,
    ep_send, frag, acc, sib_send_b, sib_recv_b, rem_send_b, rem_recv_b, ret_send, ret,
    state_r, state_i, next_r, next_i, pad_r, pad_i, w_in, w_glu, w_out, w_gate, w_up, w_down,
    load_sem, store_sem, s1, r1, s2, r2, s3, r3, s4, r4, s5, r5, s6, r6, s7, r7, s8, r8, s9, r9,
):
    e = lax.axis_index("ep")
    t = lax.axis_index("tp")
    core = lax.rem(t, 2)
    chip = t // 2
    sib = t + 1 - 2 * core
    chips = n_tp // 2
    rows, feat = tok.shape
    width = in_weight.shape[0]
    groups, states = eig_real.shape
    group_width = in_real.shape[1]
    exp_dev = gate_weight.shape[0]
    per_ep = exp_dev * capacity
    slots = n_ep * per_ep
    dim = feat * n_tp

    loads = []
    for at, (src, dst) in enumerate((
        (in_weight, w_in), (state_real, state_r), (state_imag, state_i), (glu_weight, w_glu),
        (out_weight, w_out), (gate_weight, w_gate), (up_weight, w_up), (down_weight, w_down),
    )):
        load = pltpu.make_async_copy(src, dst, load_sem.at[at])
        load.start()
        loads.append(load)

    def remote_chip(j):
        return lax.rem(chip + j, chips)

    barrier = pltpu.get_barrier_semaphore()
    greeted = [(e, sib)]
    greeted += [(e, 2 * remote_chip(j) + core) for j in range(1, chips)]
    greeted += [(lax.rem(e + k, n_ep), t) for k in range(1, n_ep)]
    for other in greeted:
        pl.semaphore_signal(barrier, inc=1, device_id=other, device_id_type=MESH)
    pl.semaphore_wait(barrier, len(greeted))

    sends = []

    def send(src, dst, send_sem, recv_sem, target):
        copy = pltpu.make_async_remote_copy(
            src_ref=src, dst_ref=dst, send_sem=send_sem, recv_sem=recv_sem,
            device_id=target, device_id_type=MESH,
        )
        copy.start()
        sends.append(copy)

    def arrive(dst, send_sem, recv_sem):
        pltpu.make_async_remote_copy(
            src_ref=dst, dst_ref=dst, send_sem=send_sem, recv_sem=recv_sem,
            device_id=(e, sib), device_id_type=MESH,
        ).wait_recv()

    def gather_send(src, dst_at, ssem, rsem):
        for j in range(1, chips):
            send(src, dst_at(t), ssem(j), rsem(t), (e, 2 * remote_chip(j) + core))
        send(src, dst_at(t), ssem(0), rsem(t), (e, sib))

    gather_send(tok, lambda p: tok_all.at[p], lambda i: s1.at[i], lambda p: r1.at[p])

    spread = (
        lax.broadcasted_iota(jnp.int32, (group_width, width), 1) % group_width
        == lax.broadcasted_iota(jnp.int32, (group_width, width), 0)
    ).astype(F32).astype(BF16)
    own_group = (
        lax.broadcasted_iota(jnp.int32, (groups * states, width), 1) // group_width
        == lax.broadcasted_iota(jnp.int32, (groups * states, width), 0) // states
    )
    pad_r[...] = jnp.where(own_group, dot_nn(in_real[...].astype(BF16), spread), 0.0).astype(BF16)
    pad_i[...] = jnp.where(own_group, dot_nn(in_imag[...].astype(BF16), spread), 0.0).astype(BF16)
    square = lax.broadcasted_iota(jnp.int32, (groups, groups), 0) == lax.broadcasted_iota(
        jnp.int32, (groups, groups), 1
    )
    time_step = jnp.exp(jnp.sum(jnp.where(square, log_step[...], 0.0), axis=1, keepdims=True))
    e_r, e_i = eig_real[...], eig_imag[...]
    magnitude = jnp.exp(e_r * time_step)
    angle = e_i * time_step
    bar_r = magnitude * jnp.cos(angle)
    bar_i = magnitude * jnp.sin(angle)
    modulus = e_r * e_r + e_i * e_i
    fac_r = ((bar_r - 1.0) * e_r + bar_i * e_i) / modulus
    fac_i = (bar_i * e_r - (bar_r - 1.0) * e_i) / modulus

    experts = exp_dev * n_ep
    lane_expert = lax.broadcasted_iota(jnp.int32, (rows, experts), 1)
    route = routes[...]
    top = route.shape[1]
    picks = [(route[:, k : k + 1] == lane_expert).astype(F32) for k in range(top)]
    earlier = (
        lax.broadcasted_iota(jnp.int32, (rows, rows), 0) > lax.broadcasted_iota(jnp.int32, (rows, rows), 1)
    ).astype(F32).astype(BF16)
    prefix = dot_nn(earlier, sum(picks[1:], picks[0]).astype(BF16))
    lane_slot = lax.broadcasted_iota(jnp.int32, (rows, slots), 1)
    choose = []
    for k in range(top):
        rank = jnp.sum(prefix * picks[k], axis=1, keepdims=True).astype(jnp.int32)
        slot = route[:, k : k + 1] * capacity + rank
        choose.append((slot == lane_slot).astype(F32))
    dispatch = jnp.transpose(sum(choose[1:], choose[0])).astype(BF16)
    choose = [one.astype(BF16) for one in choose]

    def columns(p):
        return pl.ds(pl.multiple_of(p * feat, feat), feat)

    def in_piece(p, x, total, sq):
        xf = x.astype(F32)
        sq = sq + jnp.sum(xf * xf, axis=1, keepdims=True)
        y = (xf * mix_gain[:, columns(p)].astype(F32)).astype(BF16)
        return total + dot_nt(y, w_in[:, columns(p)]), sq

    loads[0].wait()
    total, sq = in_piece(t, tok[...], jnp.zeros((rows, width), F32), jnp.zeros((rows, 1), F32))
    arrive(tok_all.at[sib], s1.at[0], r1.at[sib])
    total, sq = in_piece(sib, tok_all[sib], total, sq)
    for j in range(1, chips):
        p = 2 * remote_chip(j) + core
        arrive(tok_all.at[p], s1.at[0], r1.at[p])
        send(tok_all.at[p], tok_all.at[p], s1.at[chips + j - 1], r1.at[p], (e, sib))
        total, sq = in_piece(p, tok_all[p], total, sq)
    for j in range(1, chips):
        p = 2 * remote_chip(j) + 1 - core
        arrive(tok_all.at[p], s1.at[0], r1.at[p])
        total, sq = in_piece(p, tok_all[p], total, sq)
    driven = (total * lax.rsqrt(sq / dim + norm_eps)).astype(BF16)
    driven_f = driven.astype(F32)

    loads[1].wait()
    loads[2].wait()
    readout = skip_weight[...] * driven_f
    c_r, c_i = out_real[...], out_imag[...]
    row_group = lax.broadcasted_iota(jnp.int32, c_r.shape, 0) // group_width
    for g in range(groups):
        at = pl.ds(g, rows, stride=groups)
        part = slice(g * states, (g + 1) * states)
        push_r = dot_nt(driven, pad_r[part, :])
        push_i = dot_nt(driven, pad_i[part, :])
        old_r, old_i = state_r[at, :], state_i[at, :]
        br, bi = bar_r[g : g + 1, :], bar_i[g : g + 1, :]
        fr, fi = fac_r[g : g + 1, :], fac_i[g : g + 1, :]
        now_r = br * old_r - bi * old_i + (fr * push_r - fi * push_i)
        now_i = br * old_i + bi * old_r + (fr * push_i + fi * push_r)
        next_r[at, :] = now_r
        next_i[at, :] = now_i
        mine = row_group == g
        readout = readout + dot_nt(now_r.astype(BF16), jnp.where(mine, c_r, 0.0).astype(BF16))
        readout = readout - dot_nt(now_i.astype(BF16), jnp.where(mine, c_i, 0.0).astype(BF16))
    activated = jax.nn.gelu(readout).astype(BF16)

    act_all[t] = activated
    gather_send(act_all.at[t], lambda p: act_all.at[p], lambda i: s2.at[i], lambda p: r2.at[p])
    stores = []
    for at, (src, dst) in enumerate(((next_r, new_real), (next_i, new_imag))):
        store = pltpu.make_async_copy(src, dst, store_sem.at[at])
        store.start()
        stores.append(store)
    loads[3].wait()
    arrive(act_all.at[sib], s2.at[0], r2.at[sib])
    for j in range(1, chips):
        p = 2 * remote_chip(j) + core
        arrive(act_all.at[p], s2.at[0], r2.at[p])
        send(act_all.at[p], act_all.at[p], s2.at[chips + j - 1], r2.at[p], (e, sib))
    for j in range(1, chips):
        p = 2 * remote_chip(j) + 1 - core
        arrive(act_all.at[p], s2.at[0], r2.at[p])
    gate_pre = glu_bias[...] + jnp.zeros((rows, width), F32)
    for p in range(n_tp):
        gate_pre = gate_pre + dot_nt(act_all[p], w_glu[:, p * width : (p + 1) * width])
    glued = (activated.astype(F32) * jax.nn.sigmoid(gate_pre)).astype(BF16)

    def reduce_blocks(partial, sib_send, sib_recv, rem_send, rem_recv, ssem, rsem, ssem2, rsem2):
        order = list(range(1, chips)) + [0]
        for j in order:
            sib_send[j] = partial(2 * remote_chip(j) + 1 - core).astype(BF16)
            send(sib_send.at[j], sib_recv.at[j], ssem.at[j], rsem.at[j], (e, sib))
        for j in order[:-1]:
            p = 2 * remote_chip(j) + core
            value = partial(p)
            arrive(sib_recv.at[j], ssem.at[j], rsem.at[j])
            rem_send[j] = (value + sib_recv[j].astype(F32)).astype(BF16)
            send(rem_send.at[j], rem_recv.at[j], ssem2.at[j], rsem2.at[j], (e, p))
        value = partial(t)
        arrive(sib_recv.at[0], ssem.at[0], rsem.at[0])
        value = value + sib_recv[0].astype(F32)
        for j in order[:-1]:
            arrive(rem_recv.at[j], ssem2.at[j], rsem2.at[j])
            value = value + rem_recv[j].astype(F32)
        return value

    loads[4].wait()
    mixed = reduce_blocks(
        lambda p: dot_nn(glued, w_out[:, columns(p)]),
        sib_send_a, sib_recv_a, rem_send_a, rem_recv_a, s3, r3, s4, r4,
    )
    residual = (tok[...].astype(F32) + mixed).astype(BF16)

    packed = dot_nn(dispatch, residual).astype(BF16).reshape(n_ep, per_ep, feat)
    ep_send[...] = packed
    for k in range(1, n_ep):
        to = lax.rem(e + k, n_ep)
        send(ep_send.at[to], frag.at[t, e], s5.at[k], r5.at[e], (to, t))
    frag[t, e] = ep_send[e]
    sources = [lax.rem(e + n_ep - k, n_ep) for k in range(n_ep)]
    for k, source in enumerate(sources):
        if k:
            arrive(frag.at[t, source], s5.at[0], r5.at[source])
        gather_send(
            frag.at[t, source], lambda p: frag.at[p, source],
            lambda i: s6.at[i, k], lambda p: r6.at[p, source],
        )

    for load in loads[5:]:
        load.wait()

    def expert_piece(p, sq, first):
        xf = frag[p].reshape(slots, feat).astype(F32)
        y = (xf * moe_gain[:, columns(p)].astype(F32)).astype(BF16)
        for x in range(exp_dev):
            gate = dot_nt(y, w_gate[x, :, columns(p)])
            up = dot_nt(y, w_up[x, :, columns(p)])
            acc[2 * x] = gate if first else acc[2 * x] + gate
            acc[2 * x + 1] = up if first else acc[2 * x + 1] + up
        return sq + jnp.sum(xf * xf, axis=1, keepdims=True)

    sq = expert_piece(t, jnp.zeros((slots, 1), F32), True)
    for source in sources:
        arrive(frag.at[sib, source], s6.at[0, 0], r6.at[sib, source])
    sq = expert_piece(sib, sq, False)
    for j in range(1, chips):
        p = 2 * remote_chip(j) + core
        for k, source in enumerate(sources):
            arrive(frag.at[p, source], s6.at[0, 0], r6.at[p, source])
            send(frag.at[p, source], frag.at[p, source], s6.at[chips + j - 1, k], r6.at[p, source], (e, sib))
        sq = expert_piece(p, sq, False)
    for j in range(1, chips):
        p = 2 * remote_chip(j) + 1 - core
        for source in sources:
            arrive(frag.at[p, source], s6.at[0, 0], r6.at[p, source])
        sq = expert_piece(p, sq, False)

    second_scale = lax.rsqrt(sq / dim + norm_eps)
    hidden_of = []
    for x in range(exp_dev):
        slot_row = lax.broadcasted_iota(jnp.int32, acc.shape[1:], 0)
        mine = (slot_row % per_ep) // capacity == x
        hidden = jax.nn.silu(acc[2 * x] * second_scale) * (acc[2 * x + 1] * second_scale)
        hidden_of.append(jnp.where(mine, hidden, 0.0).astype(BF16))

    def down(p):
        value = dot_nn(hidden_of[0], w_down[0, :, columns(p)])
        for x in range(1, exp_dev):
            value = value + dot_nn(hidden_of[x], w_down[x, :, columns(p)])
        return value

    summed = reduce_blocks(
        down, sib_send_b, sib_recv_b, rem_send_b, rem_recv_b, s7, r7, s8, r8,
    ).astype(BF16)

    ret_send[...] = summed.reshape(n_ep, per_ep, feat)
    for k in range(1, n_ep):
        to = lax.rem(e + k, n_ep)
        send(ret_send.at[to], ret.at[e], s9.at[k], r9.at[e], (to, t))
    ret[e] = ret_send[e]
    for source in sources[1:]:
        arrive(ret.at[source], s9.at[0], r9.at[source])
    returned = ret[...].reshape(slots, feat)
    total = residual.astype(F32)
    weights = route_weight[...]
    for k in range(top):
        total = total + weights[:, k : k + 1] * dot_nn(choose[k], returned)
    result[...] = total.astype(BF16)

    for store in stores:
        store.wait()
    for copy in sends:
        copy.wait_send()


def local(
    tokens, state_real, state_imag, mix_gain, in_weight, eig_real, eig_imag, log_step,
    input_real, input_imag, output_matrix_real, output_matrix_imag, skip_weight,
    glu_weight, glu_bias, out_weight, moe_gain, routes, route_weight,
    gate_weight, up_weight, down_weight,
):
    rows, feat = tokens.shape
    n_ep = lax.axis_size("ep")
    n_tp = lax.axis_size("tp")
    chips = n_tp // 2
    groups, states, group_width = input_real.shape
    width = in_weight.shape[0]
    exp_dev, hidden, dim = gate_weight.shape
    experts = exp_dev * n_ep
    top_count = routes.shape[1]
    capacity = max(2, (3 * top_count * rows + 2 * experts - 1) // (2 * experts))
    per_ep = exp_dev * capacity
    slots = n_ep * per_ep
    vmem = pl.BlockSpec(memory_space=pltpu.VMEM)
    hbm = pl.BlockSpec(memory_space=pl.ANY)
    dma = pltpu.SemaphoreType.DMA
    state_shape = (rows * groups, states)
    outs = pl.pallas_call(
        functools.partial(layer_kernel, n_ep, n_tp, capacity),
        out_shape=(
            jax.ShapeDtypeStruct((rows, feat), BF16),
            jax.ShapeDtypeStruct(state_shape, F32),
            jax.ShapeDtypeStruct(state_shape, F32),
        ),
        in_specs=[vmem] * 14 + [hbm] * 8,
        out_specs=(vmem, hbm, hbm),
        scratch_shapes=[
            pltpu.VMEM((n_tp, rows, feat), BF16),
            pltpu.VMEM((n_tp, rows, width), BF16),
            pltpu.VMEM((chips, rows, feat), BF16),
            pltpu.VMEM((chips, rows, feat), BF16),
            pltpu.VMEM((chips, rows, feat), BF16),
            pltpu.VMEM((chips, rows, feat), BF16),
            pltpu.VMEM((n_ep, per_ep, feat), BF16),
            pltpu.VMEM((n_tp, n_ep, per_ep, feat), BF16),
            pltpu.VMEM((2 * exp_dev, slots, hidden), F32),
            pltpu.VMEM((chips, slots, feat), BF16),
            pltpu.VMEM((chips, slots, feat), BF16),
            pltpu.VMEM((chips, slots, feat), BF16),
            pltpu.VMEM((chips, slots, feat), BF16),
            pltpu.VMEM((n_ep, per_ep, feat), BF16),
            pltpu.VMEM((n_ep, per_ep, feat), BF16),
            pltpu.VMEM(state_shape, F32),
            pltpu.VMEM(state_shape, F32),
            pltpu.VMEM(state_shape, F32),
            pltpu.VMEM(state_shape, F32),
            pltpu.VMEM((groups * states, width), BF16),
            pltpu.VMEM((groups * states, width), BF16),
            pltpu.VMEM(in_weight.shape, BF16),
            pltpu.VMEM(glu_weight.shape, BF16),
            pltpu.VMEM(out_weight.shape, BF16),
            pltpu.VMEM(gate_weight.shape, BF16),
            pltpu.VMEM(up_weight.shape, BF16),
            pltpu.VMEM(down_weight.shape, BF16),
            dma((8,)),
            dma((2,)),
            dma((n_tp,)), dma((n_tp,)),
            dma((n_tp,)), dma((n_tp,)),
            dma((chips,)), dma((chips,)),
            dma((chips,)), dma((chips,)),
            dma((n_ep,)), dma((n_ep,)),
            dma((n_tp, n_ep)), dma((n_tp, n_ep)),
            dma((chips,)), dma((chips,)),
            dma((chips,)), dma((chips,)),
            dma((n_ep,)), dma((n_ep,)),
        ],
        compiler_params=pltpu.CompilerParams(
            collective_id=0, has_side_effects=True, vmem_limit_bytes=60 * 1024 * 1024
        ),
    )(
        tokens, mix_gain.reshape(1, dim), moe_gain.reshape(1, dim), routes, route_weight,
        eig_real, eig_imag, log_step.reshape(1, groups),
        input_real.reshape(groups * states, group_width),
        input_imag.reshape(groups * states, group_width),
        output_matrix_real.reshape(width, states), output_matrix_imag.reshape(width, states),
        skip_weight.reshape(1, width), glu_bias.reshape(1, width),
        state_real.reshape(state_shape), state_imag.reshape(state_shape),
        in_weight, glu_weight, out_weight, gate_weight, up_weight, down_weight,
    )
    result, new_real, new_imag = outs
    return result, new_real.reshape(state_real.shape), new_imag.reshape(state_imag.shape)


def solution(mesh):
    return jax.shard_map(
        local,
        mesh=mesh,
        in_specs=(
            P("ep", "tp"),
            P("ep", "tp", None),
            P("ep", "tp", None),
            P(),
            P("tp", None),
            P("tp", None),
            P("tp", None),
            P("tp"),
            P("tp", None, None),
            P("tp", None, None),
            P("tp", None, None),
            P("tp", None, None),
            P("tp"),
            P("tp", None),
            P("tp"),
            P("tp", None),
            P(),
            P("ep", None),
            P("ep", None),
            P("ep", "tp", None),
            P("ep", "tp", None),
            P("ep", "tp", None),
        ),
        out_specs=(P("ep", "tp"), P("ep", "tp", None), P("ep", "tp", None)),
        check_vma=False,
    )
```

```python
import functools

import jax
import jax.numpy as jnp
from jax import lax
from jax.experimental import pallas as pl
from jax.experimental.pallas import tpu as pltpu
from jax.sharding import PartitionSpec as P

norm_eps = 1e-06
MESH = pl.DeviceIdType.MESH
F32 = jnp.float32
BF16 = jnp.bfloat16


def dot_nt(a, b):
    return lax.dot_general(a, b, (((1,), (1,)), ((), ())), preferred_element_type=F32)


def dot_nn(a, b):
    return lax.dot_general(a, b, (((1,), (0,)), ((), ())), preferred_element_type=F32)


def layer_kernel(
    n_ep, n_tp, capacity,
    tok, mix_gain, moe_gain, routes, route_weight, eig_real, eig_imag, log_step,
    in_real, in_imag, out_real, out_imag, skip_weight, glu_bias,
    state_real, state_imag, in_weight, glu_weight, out_weight, gate_weight, up_weight, down_weight,
    result, new_real, new_imag,
    tok_all, act_all, sib_send_a, sib_recv_a, rem_send_a, rem_recv_a,
    ep_send, frag, acc, sib_send_b, sib_recv_b, rem_send_b, rem_recv_b, ret_send, ret,
    state_r, state_i, next_r, next_i, w_in, w_glu, w_out, w_gate, w_up, w_down,
    load_sem, store_sem, s1, r1, s2, r2, s3, r3, s4, r4, s5, r5, s6, r6, s7, r7, s8, r8, s9, r9,
):
    e = lax.axis_index("ep")
    t = lax.axis_index("tp")
    core = lax.rem(t, 2)
    chip = t // 2
    sib = t + 1 - 2 * core
    chips = n_tp // 2
    rows, feat = tok.shape
    width = in_weight.shape[0]
    groups, states = eig_real.shape
    group_width = width // groups
    exp_dev = gate_weight.shape[0]
    per_ep = exp_dev * capacity
    slots = n_ep * per_ep
    dim = feat * n_tp

    loads = []
    for at, (src, dst) in enumerate((
        (in_weight, w_in), (state_real, state_r), (state_imag, state_i), (glu_weight, w_glu),
        (out_weight, w_out), (gate_weight, w_gate), (up_weight, w_up), (down_weight, w_down),
    )):
        load = pltpu.make_async_copy(src, dst, load_sem.at[at])
        load.start()
        loads.append(load)

    def remote_chip(j):
        if chips & (chips - 1):
            return lax.rem(chip + j, chips)
        other, bit = chip, 1
        while bit < chips:
            if j & bit:
                other = other + bit * (1 - 2 * ((chip // bit) % 2))
            bit *= 2
        return other

    barrier = pltpu.get_barrier_semaphore()
    greeted = [(e, sib)]
    greeted += [(e, 2 * remote_chip(j) + core) for j in range(1, chips)]
    greeted += [(lax.rem(e + k, n_ep), t) for k in range(1, n_ep)]
    for other in greeted:
        pl.semaphore_signal(barrier, inc=1, device_id=other, device_id_type=MESH)
    pl.semaphore_wait(barrier, len(greeted))

    sends = []

    def send(src, dst, send_sem, recv_sem, target):
        copy = pltpu.make_async_remote_copy(
            src_ref=src, dst_ref=dst, send_sem=send_sem, recv_sem=recv_sem,
            device_id=target, device_id_type=MESH,
        )
        copy.start()
        sends.append(copy)

    def arrive(dst, send_sem, recv_sem):
        pltpu.make_async_remote_copy(
            src_ref=dst, dst_ref=dst, send_sem=send_sem, recv_sem=recv_sem,
            device_id=(e, sib), device_id_type=MESH,
        ).wait_recv()

    def gather_send(src, dst_at, ssem, rsem):
        for j in range(1, chips):
            send(src, dst_at(t), ssem(j), rsem(t), (e, 2 * remote_chip(j) + core))
        send(src, dst_at(t), ssem(0), rsem(t), (e, sib))

    gather_send(tok, lambda p: tok_all.at[p], lambda i: s1.at[i], lambda p: r1.at[p])

    square = lax.broadcasted_iota(jnp.int32, (groups, groups), 0) == lax.broadcasted_iota(
        jnp.int32, (groups, groups), 1
    )
    time_step = jnp.exp(jnp.sum(jnp.where(square, log_step[...], 0.0), axis=1, keepdims=True))
    e_r, e_i = eig_real[...], eig_imag[...]
    magnitude = jnp.exp(e_r * time_step)
    angle = e_i * time_step
    bar_r = magnitude * jnp.cos(angle)
    bar_i = magnitude * jnp.sin(angle)
    modulus = e_r * e_r + e_i * e_i
    fac_r = ((bar_r - 1.0) * e_r + bar_i * e_i) / modulus
    fac_i = (bar_i * e_r - (bar_r - 1.0) * e_i) / modulus

    experts = exp_dev * n_ep
    lane_expert = lax.broadcasted_iota(jnp.int32, (rows, experts), 1)
    top = routes.shape[0]
    token_square = lax.broadcasted_iota(jnp.int32, (rows, rows), 0) == lax.broadcasted_iota(
        jnp.int32, (rows, rows), 1
    )

    def column(row):
        return jnp.sum(jnp.where(token_square, row.astype(F32), 0.0), axis=1, keepdims=True)

    route = [column(routes[k : k + 1, :]).astype(jnp.int32) for k in range(top)]
    weights = [column(route_weight[k : k + 1, :]) for k in range(top)]
    picks = [(route[k] == lane_expert).astype(F32) for k in range(top)]
    earlier = (
        lax.broadcasted_iota(jnp.int32, (rows, rows), 0) > lax.broadcasted_iota(jnp.int32, (rows, rows), 1)
    ).astype(F32).astype(BF16)
    prefix = dot_nn(earlier, sum(picks[1:], picks[0]).astype(BF16))
    lane_slot = lax.broadcasted_iota(jnp.int32, (rows, slots), 1)
    choose = []
    for k in range(top):
        rank = jnp.sum(prefix * picks[k], axis=1, keepdims=True).astype(jnp.int32)
        slot = route[k] * capacity + rank
        choose.append((slot == lane_slot).astype(F32))
    dispatch = jnp.transpose(sum(choose[1:], choose[0])).astype(BF16)
    choose = [one.astype(BF16) for one in choose]

    def columns(p):
        return pl.ds(pl.multiple_of(p * feat, feat), feat)

    def gain_row(gain, p):
        if gain.ndim == 2:
            return gain[:, columns(p)].astype(F32)
        return gain[columns(p)].astype(F32).reshape(1, feat)

    def in_piece(p, x, total, sq):
        xf = x.astype(F32)
        sq = sq + jnp.sum(xf * xf, axis=1, keepdims=True)
        y = (xf * gain_row(mix_gain, p)).astype(BF16)
        return total + dot_nt(y, w_in[:, columns(p)]), sq

    loads[0].wait()
    total, sq = in_piece(t, tok[...], jnp.zeros((rows, width), F32), jnp.zeros((rows, 1), F32))
    arrive(tok_all.at[sib], s1.at[0], r1.at[sib])
    total, sq = in_piece(sib, tok_all[sib], total, sq)
    for j in range(1, chips):
        p = 2 * remote_chip(j) + core
        arrive(tok_all.at[p], s1.at[0], r1.at[p])
        send(tok_all.at[p], tok_all.at[p], s1.at[chips + j - 1], r1.at[p], (e, sib))
        total, sq = in_piece(p, tok_all[p], total, sq)
    for j in range(1, chips):
        p = 2 * remote_chip(j) + 1 - core
        arrive(tok_all.at[p], s1.at[0], r1.at[p])
        total, sq = in_piece(p, tok_all[p], total, sq)
    driven = (total * lax.rsqrt(sq / dim + norm_eps)).astype(BF16)
    driven_f = driven.astype(F32)

    loads[1].wait()
    loads[2].wait()
    readout = skip_weight[...] * driven_f
    c_r, c_i = out_real[...], out_imag[...]
    b_r, b_i = in_real[...], in_imag[...]
    row_group = lax.broadcasted_iota(jnp.int32, c_r.shape, 0) // group_width
    for g in range(groups):
        at = pl.ds(g, rows, stride=groups)
        mine = row_group == g
        push_r = dot_nn(driven, jnp.where(mine, b_r, 0.0).astype(BF16))
        push_i = dot_nn(driven, jnp.where(mine, b_i, 0.0).astype(BF16))
        old_r, old_i = state_r[at, :], state_i[at, :]
        br, bi = bar_r[g : g + 1, :], bar_i[g : g + 1, :]
        fr, fi = fac_r[g : g + 1, :], fac_i[g : g + 1, :]
        now_r = br * old_r - bi * old_i + (fr * push_r - fi * push_i)
        now_i = br * old_i + bi * old_r + (fr * push_i + fi * push_r)
        next_r[at, :] = now_r
        next_i[at, :] = now_i
        readout = readout + dot_nt(now_r.astype(BF16), jnp.where(mine, c_r, 0.0).astype(BF16))
        readout = readout - dot_nt(now_i.astype(BF16), jnp.where(mine, c_i, 0.0).astype(BF16))
    activated = jax.nn.gelu(readout).astype(BF16)

    act_all[t] = activated
    gather_send(act_all.at[t], lambda p: act_all.at[p], lambda i: s2.at[i], lambda p: r2.at[p])
    stores = []
    for at, (src, dst) in enumerate(((next_r, new_real), (next_i, new_imag))):
        store = pltpu.make_async_copy(src, dst, store_sem.at[at])
        store.start()
        stores.append(store)
    loads[3].wait()
    arrive(act_all.at[sib], s2.at[0], r2.at[sib])
    for j in range(1, chips):
        p = 2 * remote_chip(j) + core
        arrive(act_all.at[p], s2.at[0], r2.at[p])
        send(act_all.at[p], act_all.at[p], s2.at[chips + j - 1], r2.at[p], (e, sib))
    for j in range(1, chips):
        p = 2 * remote_chip(j) + 1 - core
        arrive(act_all.at[p], s2.at[0], r2.at[p])
    gate_pre = glu_bias[...] + jnp.zeros((rows, width), F32)
    for p in range(n_tp):
        gate_pre = gate_pre + dot_nt(act_all[p], w_glu[:, p * width : (p + 1) * width])
    glued = (activated.astype(F32) * jax.nn.sigmoid(gate_pre)).astype(BF16)

    def reduce_blocks(partial, sib_send, sib_recv, rem_send, rem_recv, ssem, rsem, ssem2, rsem2):
        order = list(range(1, chips)) + [0]
        for j in order:
            sib_send[j] = partial(2 * remote_chip(j) + 1 - core).astype(BF16)
            send(sib_send.at[j], sib_recv.at[j], ssem.at[j], rsem.at[j], (e, sib))
        for j in order[:-1]:
            p = 2 * remote_chip(j) + core
            value = partial(p)
            arrive(sib_recv.at[j], ssem.at[j], rsem.at[j])
            rem_send[j] = (value + sib_recv[j].astype(F32)).astype(BF16)
            send(rem_send.at[j], rem_recv.at[j], ssem2.at[j], rsem2.at[j], (e, p))
        value = partial(t)
        arrive(sib_recv.at[0], ssem.at[0], rsem.at[0])
        value = value + sib_recv[0].astype(F32)
        for j in order[:-1]:
            arrive(rem_recv.at[j], ssem2.at[j], rsem2.at[j])
            value = value + rem_recv[j].astype(F32)
        return value

    loads[4].wait()
    mixed = reduce_blocks(
        lambda p: dot_nn(glued, w_out[:, columns(p)]),
        sib_send_a, sib_recv_a, rem_send_a, rem_recv_a, s3, r3, s4, r4,
    )
    residual = (tok[...].astype(F32) + mixed).astype(BF16)

    packed = dot_nn(dispatch, residual).astype(BF16).reshape(n_ep, per_ep, feat)
    ep_send[...] = packed
    for k in range(1, n_ep):
        to = lax.rem(e + k, n_ep)
        send(ep_send.at[to], frag.at[t, e], s5.at[k], r5.at[e], (to, t))
    frag[t, e] = ep_send[e]
    sources = [lax.rem(e + n_ep - k, n_ep) for k in range(n_ep)]
    for k, source in enumerate(sources):
        if k:
            arrive(frag.at[t, source], s5.at[0], r5.at[source])
        gather_send(
            frag.at[t, source], lambda p: frag.at[p, source],
            lambda i: s6.at[i, k], lambda p: r6.at[p, source],
        )

    for load in loads[5:]:
        load.wait()

    def expert_piece(p, sq, first):
        xf = frag[p].reshape(slots, feat).astype(F32)
        y = (xf * gain_row(moe_gain, p)).astype(BF16)
        for x in range(exp_dev):
            gate = dot_nt(y, w_gate[x, :, columns(p)])
            up = dot_nt(y, w_up[x, :, columns(p)])
            acc[2 * x] = gate if first else acc[2 * x] + gate
            acc[2 * x + 1] = up if first else acc[2 * x + 1] + up
        return sq + jnp.sum(xf * xf, axis=1, keepdims=True)

    sq = expert_piece(t, jnp.zeros((slots, 1), F32), True)
    for source in sources:
        arrive(frag.at[sib, source], s6.at[0, 0], r6.at[sib, source])
    sq = expert_piece(sib, sq, False)
    for j in range(1, chips):
        p = 2 * remote_chip(j) + core
        for k, source in enumerate(sources):
            arrive(frag.at[p, source], s6.at[0, 0], r6.at[p, source])
            send(frag.at[p, source], frag.at[p, source], s6.at[chips + j - 1, k], r6.at[p, source], (e, sib))
        sq = expert_piece(p, sq, False)
    for j in range(1, chips):
        p = 2 * remote_chip(j) + 1 - core
        for source in sources:
            arrive(frag.at[p, source], s6.at[0, 0], r6.at[p, source])
        sq = expert_piece(p, sq, False)

    second_scale = lax.rsqrt(sq / dim + norm_eps)
    hidden_of = []
    for x in range(exp_dev):
        slot_row = lax.broadcasted_iota(jnp.int32, acc.shape[1:], 0)
        mine = (slot_row % per_ep) // capacity == x
        hidden = jax.nn.silu(acc[2 * x] * second_scale) * (acc[2 * x + 1] * second_scale)
        hidden_of.append(jnp.where(mine, hidden, 0.0).astype(BF16))

    def down(p):
        value = dot_nn(hidden_of[0], w_down[0, :, columns(p)])
        for x in range(1, exp_dev):
            value = value + dot_nn(hidden_of[x], w_down[x, :, columns(p)])
        return value

    summed = reduce_blocks(
        down, sib_send_b, sib_recv_b, rem_send_b, rem_recv_b, s7, r7, s8, r8,
    ).astype(BF16)

    ret_send[...] = summed.reshape(n_ep, per_ep, feat)
    for k in range(1, n_ep):
        to = lax.rem(e + k, n_ep)
        send(ret_send.at[to], ret.at[e], s9.at[k], r9.at[e], (to, t))
    ret[e] = ret_send[e]
    for source in sources[1:]:
        arrive(ret.at[source], s9.at[0], r9.at[source])
    returned = ret[...].reshape(slots, feat)
    total = residual.astype(F32)
    for k in range(top):
        total = total + weights[k] * dot_nn(choose[k], returned)
    result[...] = total.astype(BF16)

    for store in stores:
        store.wait()
    for copy in sends:
        copy.wait_send()


def hand_over(a, b, c, a_out, b_out, c_out, a_held, b_held, c_held, sem_in, sem_out):
    triples = ((a, a_held, a_out), (b, b_held, b_out), (c, c_held, c_out))
    ins = [pltpu.make_async_copy(src, held, sem_in.at[i]) for i, (src, held, _) in enumerate(triples)]
    outs = [pltpu.make_async_copy(held, dst, sem_out.at[i]) for i, (_, held, dst) in enumerate(triples)]
    for copy in ins:
        copy.start()
    for copy, back in zip(ins, outs):
        copy.wait()
        back.start()
    for back in outs:
        back.wait()


def local(
    tokens, state_real, state_imag, mix_gain, in_weight, eig_real, eig_imag, log_step,
    input_real, input_imag, output_matrix_real, output_matrix_imag, skip_weight,
    glu_weight, glu_bias, out_weight, moe_gain, routes, route_weight,
    gate_weight, up_weight, down_weight,
):
    rows, feat = tokens.shape
    n_ep = lax.axis_size("ep")
    n_tp = lax.axis_size("tp")
    chips = n_tp // 2
    groups, states, group_width = input_real.shape
    width = in_weight.shape[0]
    exp_dev, hidden, dim = gate_weight.shape
    experts = exp_dev * n_ep
    top_count = routes.shape[1]
    capacity = max(2, (3 * top_count * rows + 2 * experts - 1) // (2 * experts))
    per_ep = exp_dev * capacity
    slots = n_ep * per_ep
    vmem = pl.BlockSpec(memory_space=pltpu.VMEM)
    hbm = pl.BlockSpec(memory_space=pl.ANY)
    dma = pltpu.SemaphoreType.DMA
    state_shape = (rows * groups, states)
    if feat % 256:
        mix_gain, moe_gain = mix_gain.reshape(1, dim), moe_gain.reshape(1, dim)
    outs = pl.pallas_call(
        functools.partial(layer_kernel, n_ep, n_tp, capacity),
        out_shape=(
            jax.ShapeDtypeStruct((rows, feat), BF16),
            jax.ShapeDtypeStruct(state_shape, F32),
            jax.ShapeDtypeStruct(state_shape, F32),
        ),
        in_specs=[vmem] * 14 + [hbm] * 8,
        out_specs=(vmem, hbm, hbm),
        scratch_shapes=[
            pltpu.VMEM((n_tp, rows, feat), BF16),
            pltpu.VMEM((n_tp, rows, width), BF16),
            pltpu.VMEM((chips, rows, feat), BF16),
            pltpu.VMEM((chips, rows, feat), BF16),
            pltpu.VMEM((chips, rows, feat), BF16),
            pltpu.VMEM((chips, rows, feat), BF16),
            pltpu.VMEM((n_ep, per_ep, feat), BF16),
            pltpu.VMEM((n_tp, n_ep, per_ep, feat), BF16),
            pltpu.VMEM((2 * exp_dev, slots, hidden), F32),
            pltpu.VMEM((chips, slots, feat), BF16),
            pltpu.VMEM((chips, slots, feat), BF16),
            pltpu.VMEM((chips, slots, feat), BF16),
            pltpu.VMEM((chips, slots, feat), BF16),
            pltpu.VMEM((n_ep, per_ep, feat), BF16),
            pltpu.VMEM((n_ep, per_ep, feat), BF16),
            pltpu.VMEM(state_shape, F32),
            pltpu.VMEM(state_shape, F32),
            pltpu.VMEM(state_shape, F32),
            pltpu.VMEM(state_shape, F32),
            pltpu.VMEM(in_weight.shape, BF16),
            pltpu.VMEM(glu_weight.shape, BF16),
            pltpu.VMEM(out_weight.shape, BF16),
            pltpu.VMEM(gate_weight.shape, BF16),
            pltpu.VMEM(up_weight.shape, BF16),
            pltpu.VMEM(down_weight.shape, BF16),
            dma((8,)),
            dma((2,)),
            dma((n_tp,)), dma((n_tp,)),
            dma((n_tp,)), dma((n_tp,)),
            dma((chips,)), dma((chips,)),
            dma((chips,)), dma((chips,)),
            dma((n_ep,)), dma((n_ep,)),
            dma((n_tp, n_ep)), dma((n_tp, n_ep)),
            dma((chips,)), dma((chips,)),
            dma((chips,)), dma((chips,)),
            dma((n_ep,)), dma((n_ep,)),
        ],
        compiler_params=pltpu.CompilerParams(
            collective_id=0, has_side_effects=True, vmem_limit_bytes=60 * 1024 * 1024
        ),
    )(
        tokens, mix_gain, moe_gain, routes.T, route_weight.T,
        eig_real, eig_imag, log_step.reshape(1, groups),
        jnp.swapaxes(input_real, 1, 2).reshape(width, states),
        jnp.swapaxes(input_imag, 1, 2).reshape(width, states),
        output_matrix_real.reshape(width, states), output_matrix_imag.reshape(width, states),
        skip_weight.reshape(1, width), glu_bias.reshape(1, width),
        state_real.reshape(state_shape), state_imag.reshape(state_shape),
        in_weight, glu_weight, out_weight, gate_weight, up_weight, down_weight,
    )
    result, new_real, new_imag = pl.pallas_call(
        hand_over,
        out_shape=tuple(jax.ShapeDtypeStruct(one.shape, one.dtype) for one in outs),
        in_specs=[hbm] * 3,
        out_specs=(hbm,) * 3,
        scratch_shapes=[pltpu.VMEM(one.shape, one.dtype) for one in outs] + [dma((3,)), dma((3,))],
        compiler_params=pltpu.CompilerParams(vmem_limit_bytes=60 * 1024 * 1024),
    )(*outs)
    return result, new_real.reshape(state_real.shape), new_imag.reshape(state_imag.shape)


def solution(mesh):
    return jax.shard_map(
        local,
        mesh=mesh,
        in_specs=(
            P("ep", "tp"),
            P("ep", "tp", None),
            P("ep", "tp", None),
            P(),
            P("tp", None),
            P("tp", None),
            P("tp", None),
            P("tp"),
            P("tp", None, None),
            P("tp", None, None),
            P("tp", None, None),
            P("tp", None, None),
            P("tp"),
            P("tp", None),
            P("tp"),
            P("tp", None),
            P(),
            P("ep", None),
            P("ep", None),
            P("ep", "tp", None),
            P("ep", "tp", None),
            P("ep", "tp", None),
        ),
        out_specs=(P("ep", "tp"), P("ep", "tp", None), P("ep", "tp", None)),
        check_vma=False,
    )
```
